32 devices in a mesh: ep: 8 (over z, y), tp: 4 (over x, core).
Axes of the slice: x: 2, y: 2, z: 4, core: 2. Of those that a mesh axis runs over, the one named last changes fastest.
Arguments:
- mixer_input: bfloat16 [4096, 2048], P(('ep', 'tp')), may hold values from -6 to 6
- expert_input: bfloat16 [4096, 2048], P(('ep', 'tp')), may hold values from -6 to 6
- mixer_gain: float32 [2048], replicated, may hold values from 0.1 to 1.9
- query_down: bfloat16 [2048, 1536], replicated, may hold values from -0.125 to 0.125
- latent_down: bfloat16 [2048, 512], replicated, may hold values from -0.125 to 0.125
- rotary_down: bfloat16 [2048, 32], replicated, may hold values from -0.125 to 0.125
- query_gain: float32 [1536], replicated, may hold values from 0.8 to 40, as said below
- latent_gain: float32 [512], replicated, may hold values from 0.1 to 1.9
- query_plain: bfloat16 [1536, 1024], P(None, 'tp'), may hold values from -0.15625 to 0.15625
- query_rotary: bfloat16 [1536, 512], P(None, 'tp'), may hold values from -0.15625 to 0.15625
- key_plain: bfloat16 [512, 1024], P(None, 'tp'), may hold values from -0.25 to 0.25
- value_up: bfloat16 [512, 1024], P(None, 'tp'), may hold values from -0.25 to 0.25
- output_proj: bfloat16 [1024, 2048], P('tp'), may hold values from -0.1875 to 0.1875
- mixed_gain: float32 [2048], replicated, may hold values from 0.1 to 1.9
- expert_norm: float32 [2048], replicated, may hold values from 0.1 to 1.9
- route_ids: int32 [4096, 2], P(('ep', 'tp')), may hold values from 0 to 7, all different within a row; in each aligned block of 128 rows (0 to 127, 128 to 255, ...) at most 40 rows name the same one
- route_weight: float32 [4096, 2], P(('ep', 'tp')), may hold values from 0.2 to 1
- gate_proj: bfloat16 [8, 2048, 2048], P('ep', None, 'tp'), may hold values from -0.3984375 to 0.3984375
- up_proj: bfloat16 [8, 2048, 2048], P('ep', None, 'tp'), may hold values from -0.3984375 to 0.3984375
- down_proj: bfloat16 [8, 2048, 2048], P('ep', 'tp'), may hold values from -0.125 to 0.125
- expert_gain: float32 [2048], replicated, may hold values from 0.1 to 1.9
Outputs:
- mixer_out: bfloat16 [4096, 2048], P(('ep', 'tp'))
- expert_out: bfloat16 [4096, 2048], P(('ep', 'tp'))
The draws below stay inside these ranges and needn't reach their ends.
Inputs may be any that keep to these rules, and one draw needn't show every extreme that they name: `route_ids`: each row names 2 different experts. Within the rows of one device (128 aligned rows) no expert is named more than 40 times, a bound that some block reaches. `query_gain`: Positive.
All inputs are finite; a program needn't handle non-finite values.
Results may differ from the reference program's by a relative error of at most 0.018.
The reference program's roundings to bfloat16 on the way count: a program that leaves them out, or rounds other values in their place, can miss the bound.
Values may be sent and summed in bfloat16 or wider, within the bound.
No kernel may reach another device: no remote copies, remote signals or barrier semaphores. Data moves between devices by JAX's collectives and lax.ppermute only.
A program may use at most 128 MiB of HBM per device.

```python
import math
import jax
import jax.numpy as jnp
import numpy as np
from jax import lax

D = 2048
HEADS = 16
NOPE = 64
ROPE = 32
VDIM = 64
Q_RANK = 1536
KV_RANK = 512
FF = 2048
TOPK = 2
TOK_DEV = 128
TOKENS = 4096
EXPERTS = 8
CAP = 40
N_TP = 4


def draw_query_gain(key, part):
    return 1.0 + 0.18 * jax.random.uniform(key, (Q_RANK,), jnp.float32, -1.0, 1.0)


def steps_of(rng, shape, pieces, low, largest):
    loudness = 1.0
    for dim, parts in pieces:
        steps = jax.random.uniform(jax.random.fold_in(jax.random.fold_in(rng, 6), dim), (parts,), jnp.float32, low / len(pieces), largest / len(pieces))
        loudness = loudness * jnp.repeat(jnp.exp(steps), shape[dim] // parts).reshape((-1,) + (1,) * (len(shape) - 1 - dim))
    return loudness


def shared_out(rng, own, number, rows, amount, top, reach, skew):
    ranking = jax.random.permutation(rng, amount)
    packed, ordinary = shares(amount, rows * top, reach, skew, True), shares(amount, rows * top, reach, skew, False)
    places = jnp.arange(amount)

    def named(tallies, rotation):
        used = int((tallies > 0).sum())
        fixed = max(1, used // 4)
        passed = fixed + (places - fixed + rotation * (used - fixed)) % max(1, amount - fixed)
        return jnp.zeros((amount,), jnp.int32).at[ranking[jnp.where(places < fixed, places, passed)]].set(jnp.asarray(tallies, jnp.int32))

    tallies = jnp.where(number % 4 == 0, named(packed, number // 4), named(ordinary, number - number // 4 - 1))
    mixed = jax.random.permutation(jax.random.fold_in(own, 3), amount)
    donor, receiver = mixed[0:amount // 2 * 2:2], mixed[1:amount // 2 * 2:2]
    margin = jnp.minimum(tallies[donor] - 1, reach - tallies[receiver]) // 2
    margin = jnp.where((donor == ranking[0]) | (receiver == ranking[0]) | (tallies[receiver] == 0), 0, jnp.maximum(margin, 0))
    passed = jax.random.randint(jax.random.fold_in(own, 4), (amount // 2,), 0, 1 << 20) % (margin + 1)
    tallies = tallies.at[donor].add(-passed).at[receiver].add(passed)
    members = jnp.searchsorted(jnp.cumsum(tallies), jnp.arange(rows * top), side="right").astype(jnp.int32)
    grid = members.reshape(top, rows).T
    grid = grid[jax.random.permutation(jax.random.fold_in(own, 1), rows)]
    rotation = jax.random.randint(jax.random.fold_in(own, 2), (rows, 1), 0, top)
    return jnp.take_along_axis(grid, (jnp.arange(top)[None, :] + rotation) % top, axis=1)


def shares(count, total, most, slope, full):
    portions = [(1 << 20) // math.isqrt(rank ** slope) + 1 for rank in range(1, count + 1)]
    largest = most if full else min(most, max(-(-total // count), total * portions[0] // sum(portions)))
    least = 1 if total - largest >= count - 1 else 0
    holding, spare = [largest] + [least] * (count - 1), total - largest - least * (count - 1)
    while spare > 0:
        movable = [i for i in range(1, count) if holding[i] < largest] or [i for i in range(1, count) if holding[i] < most]
        mass, remaining = sum([portions[i] for i in movable]), spare
        for i in movable:
            more = min(most - holding[i], max(1, remaining * portions[i] // mass), spare)
            holding[i] = holding[i] + more
            spare = spare - more
    return np.array(holding)


def normal_values(key, extent, deviation, most, pieces=(), held_as=jnp.bfloat16):
    values = deviation * jax.random.normal(key, extent, jnp.float32)
    if pieces:
        values = values * steps_of(key, extent, pieces, -0.22, 0.18)
    return jnp.clip(values, -most, most).astype(held_as)


def setup_inputs(seed: int = 0) -> dict:
    streams_of = jax.random.split(jax.random.key(seed), 22)
    mixer_input = normal_values(streams_of[0], (TOKENS, D), 1.0, 6.0, ((0, 32),))
    expert_input = normal_values(streams_of[1], (TOKENS, D), 1.0, 6.0, ((0, 32),))
    mixer_gain = jnp.clip(1.0 + 0.18 * jax.random.normal(streams_of[2], (D,), jnp.float32), 0.1, 1.9)
    query_down = normal_values(streams_of[3], (D, Q_RANK), D ** -0.5, 0.125)
    latent_down = normal_values(streams_of[4], (D, KV_RANK), D ** -0.5, 0.125)
    rotary_down = normal_values(streams_of[5], (D, ROPE), D ** -0.5, 0.125)
    query_gain = draw_query_gain(jax.random.fold_in(streams_of[21], 71), 0)
    latent_gain = jnp.clip(1.0 + 0.18 * jax.random.normal(streams_of[7], (KV_RANK,), jnp.float32), 0.1, 1.9)
    query_plain = normal_values(streams_of[8], (Q_RANK, HEADS * NOPE), Q_RANK ** -0.5, 0.15625, ((1, 4),))
    query_rotary = normal_values(streams_of[9], (Q_RANK, HEADS * ROPE), Q_RANK ** -0.5, 0.15625, ((1, 4),))
    key_plain = normal_values(streams_of[10], (KV_RANK, HEADS * NOPE), KV_RANK ** -0.5, 0.25, ((1, 4),))
    value_up = normal_values(streams_of[11], (KV_RANK, HEADS * VDIM), KV_RANK ** -0.5, 0.25, ((1, 4),))
    output_proj = normal_values(streams_of[12], (HEADS * VDIM, D), (HEADS * VDIM) ** -0.5, 0.1875, ((0, 4),))
    mixed_gain = jnp.clip(1.0 + 0.18 * jax.random.normal(streams_of[13], (D,), jnp.float32), 0.1, 1.9)
    expert_norm = jnp.clip(1.0 + 0.18 * jax.random.normal(streams_of[14], (D,), jnp.float32), 0.1, 1.9)
    route_ids_keys = jax.random.split(jax.random.fold_in(streams_of[15], 1), TOKENS // TOK_DEV)
    route_ids_turns = jax.random.permutation(jax.random.fold_in(streams_of[15], 3), TOKENS // TOK_DEV)
    route_ids = jax.vmap(lambda own, number: shared_out(jax.random.fold_in(streams_of[15], 2), own, number, TOK_DEV, EXPERTS, TOPK, CAP, 0))(route_ids_keys, route_ids_turns).reshape((TOKENS, TOPK))
    route_weight = jnp.clip(jnp.exp(math.log(1.0) - 1.609438 * jax.random.uniform(streams_of[16], (TOKENS, TOPK), jnp.float32) ** steps_of(streams_of[16], (TOKENS, TOPK), ((0, 32),), -0.2, 0.2)), 0.2, 1.0)
    gate_proj = normal_values(streams_of[17], (EXPERTS, D, FF), 0.066, 0.3984375, ((0, 8), (2, 4)))
    up_proj = normal_values(streams_of[18], (EXPERTS, D, FF), 0.066, 0.3984375, ((0, 8), (2, 4)))
    down_proj = normal_values(streams_of[19], (EXPERTS, FF, D), FF ** -0.5, 0.125, ((0, 8), (1, 4)))
    expert_gain = jnp.clip(1.0 + 0.18 * jax.random.normal(streams_of[20], (D,), jnp.float32), 0.1, 1.9)
    return {"mixer_input": mixer_input, "expert_input": expert_input, "mixer_gain": mixer_gain, "query_down": query_down, "latent_down": latent_down, "rotary_down": rotary_down, "query_gain": query_gain, "latent_gain": latent_gain, "query_plain": query_plain, "query_rotary": query_rotary, "key_plain": key_plain, "value_up": value_up, "output_proj": output_proj, "mixed_gain": mixed_gain, "expert_norm": expert_norm, "route_ids": route_ids, "route_weight": route_weight, "gate_proj": gate_proj, "up_proj": up_proj, "down_proj": down_proj, "expert_gain": expert_gain}


EPS = 1e-06
CLAMP = 7.0
ALPHA = 1.702
THETA = 10000.0

def norm_rows(values, gain):
    values = values.astype(jnp.float32)
    scale = lax.rsqrt(lax.optimization_barrier(jnp.mean(values * values, axis=-1, keepdims=True)) + EPS)
    return values * scale * gain.astype(jnp.float32)

def rounded(values):
    return lax.optimization_barrier(values.astype(jnp.bfloat16)).astype(jnp.float32)

def turn_tables(positions, width):
    half = width // 2
    freqs = THETA ** (-2.0 * jnp.arange(half, dtype=jnp.float32) / width)
    angles = positions.astype(jnp.float32)[:, None] * freqs[None, :]
    return (jnp.cos(angles), jnp.sin(angles))

def rotate(values, cosine, sine):
    half = values.shape[-1] // 2
    first = values[..., :half]
    second = values[..., half:]
    return jnp.concatenate([first * cosine - second * sine, second * cosine + first * sine], axis=-1)

def reference(mixer_input, expert_input, mixer_gain, query_down, latent_down, rotary_down, query_gain, latent_gain, query_plain, query_rotary, key_plain, value_up, output_proj, mixed_gain, expert_norm, route_ids, route_weight, gate_proj, up_proj, down_proj, expert_gain):
    positions = jnp.arange(TOKENS, dtype=jnp.int32)
    hidden = norm_rows(mixer_input, mixer_gain).astype(jnp.bfloat16)
    query_lat = norm_rows(jnp.dot(hidden, query_down, preferred_element_type=jnp.float32), query_gain).astype(jnp.bfloat16)
    key_lat = norm_rows(jnp.dot(hidden, latent_down, preferred_element_type=jnp.float32), latent_gain).astype(jnp.bfloat16)
    cosine, sine = turn_tables(positions, ROPE)
    key_turn = rotate(jnp.dot(hidden, rotary_down, preferred_element_type=jnp.float32), cosine, sine).astype(jnp.bfloat16)
    query_nope = jnp.dot(query_lat, query_plain, preferred_element_type=jnp.float32).astype(jnp.bfloat16).reshape(TOKENS, HEADS, NOPE)
    query_pe = rotate(jnp.dot(query_lat, query_rotary, preferred_element_type=jnp.float32).reshape(TOKENS, HEADS, ROPE), cosine[:, None, :], sine[:, None, :]).astype(jnp.bfloat16)
    keys = rounded(jnp.dot(key_lat, key_plain, preferred_element_type=jnp.float32)).reshape(TOKENS, HEADS, NOPE)
    values = rounded(jnp.dot(key_lat, value_up, preferred_element_type=jnp.float32)).reshape(TOKENS, HEADS, VDIM)
    turned = key_turn.astype(jnp.float32)
    scale = (NOPE + ROPE) ** (-0.5)
    span = math.gcd(TOKENS, 128)

    def attend(block):
        plain, rotated = block
        scores = (jnp.einsum('qhd,khd->qhk', plain.astype(jnp.float32), keys) + jnp.einsum('qhr,kr->qhk', rotated.astype(jnp.float32), turned)) * scale
        peak = lax.optimization_barrier(jnp.max(scores, axis=-1, keepdims=True))
        expos = jnp.exp(scores - peak)
        totals = lax.optimization_barrier(jnp.sum(expos, axis=-1))
        summed = jnp.einsum('qhk,khd->qhd', rounded(expos), values)
        return (summed / totals[..., None]).astype(jnp.bfloat16)
    attended = lax.map(attend, (query_nope.reshape(TOKENS // span, span, HEADS, NOPE), query_pe.reshape(TOKENS // span, span, HEADS, ROPE)))
    attended = attended.reshape(TOKENS, HEADS * VDIM)
    width = HEADS * VDIM // N_TP
    mixed = jnp.zeros((TOKENS, D), jnp.float32)
    for group in range(N_TP):
        mixed = mixed + rounded(jnp.dot(attended[:, group * width:(group + 1) * width], output_proj[group * width:(group + 1) * width], preferred_element_type=jnp.float32))
    mixer_out = norm_rows(mixed, mixed_gain).astype(jnp.bfloat16)
    expert_hidden = norm_rows(expert_input, expert_norm).astype(jnp.bfloat16)
    blocks = TOKENS // TOK_DEV
    assigned = TOK_DEV * TOPK
    block_ids = route_ids.reshape(blocks, assigned)
    onehot = (block_ids[:, :, None] == jnp.arange(EXPERTS, dtype=jnp.int32)[None, None, :]).astype(jnp.int32)
    order = lax.optimization_barrier(jnp.sum((jnp.cumsum(onehot, axis=1) - onehot) * onehot, axis=2))
    slot = (jnp.arange(blocks, dtype=jnp.int32)[:, None] * CAP + order).reshape(-1).astype(jnp.int32)
    owner = (jnp.arange(blocks * assigned, dtype=jnp.int32) // TOPK).astype(jnp.int32)
    flat_ids = route_ids.reshape(-1).astype(jnp.int32)
    table = jnp.zeros((EXPERTS, blocks * CAP), jnp.int32).at[flat_ids, slot].set(owner)
    share = jnp.zeros((EXPERTS, blocks * CAP), jnp.float32).at[flat_ids, slot].set(route_weight.reshape(-1).astype(jnp.float32))
    units = FF // N_TP

    def one_expert(total, inputs):
        rows_at, weight_at, gate_w, up_w, down_w = inputs
        rows = expert_hidden[rows_at]
        gate = jnp.minimum(jnp.dot(rows, gate_w, preferred_element_type=jnp.float32), CLAMP)
        up = jnp.clip(jnp.dot(rows, up_w, preferred_element_type=jnp.float32), -CLAMP, CLAMP)
        act = ((up + 1.0) * gate * jax.nn.sigmoid(ALPHA * gate)).astype(jnp.bfloat16)
        result = jnp.zeros((rows.shape[0], D), jnp.float32)
        for group in range(N_TP):
            result = result + rounded(jnp.dot(act[:, group * units:(group + 1) * units], down_w[group * units:(group + 1) * units], preferred_element_type=jnp.float32))
        result = rounded(result)
        total = total.at[rows_at].add(result * weight_at[:, None])
        return (total, None)
    combined, _ = lax.scan(one_expert, jnp.zeros((TOKENS, D), jnp.float32), (table, share, gate_proj, up_proj, down_proj))
    expert_out = norm_rows(combined, expert_gain).astype(jnp.bfloat16)
    return (mixer_out, expert_out)
```

```python
import math

import jax
import jax.numpy as jnp
from jax import lax
from jax.experimental import pallas as pl
from jax.experimental.pallas import tpu as pltpu
from jax.sharding import PartitionSpec as P

NOPE = 64
ROPE = 32
VDIM = 64


EPS = 1e-06
CLAMP = 7.0
ALPHA = 1.702
THETA = 10000.0
LOG2E = math.log2(math.e)


def norm_rows(values, gain):
    values = values.astype(jnp.float32)
    scale = lax.rsqrt(jnp.mean(values * values, axis=-1, keepdims=True) + EPS)
    return values * scale * gain


def turn_tables(positions, width):
    half = width // 2
    freqs = THETA ** (-2.0 * jnp.arange(half, dtype=jnp.float32) / width)
    angles = positions.astype(jnp.float32)[:, None] * freqs[None, :]
    return (jnp.cos(angles), jnp.sin(angles))


def swap_with(values, axis, stride):
    count = lax.axis_size(axis)
    return lax.ppermute(values, axis, [(i, i ^ stride) for i in range(count)])


def shift_by(values, axis, step):
    count = lax.axis_size(axis)
    return lax.ppermute(values, axis, [(i, (i + step) % count) for i in range(count)])


def strides_of(axis):
    count = lax.axis_size(axis)
    return [1 << b for b in reversed(range(count.bit_length() - 1))]


def block_owners(axis):
    owners = [0]
    for stride in strides_of(axis):
        owners = owners + [o ^ stride for o in owners]
    return owners


def gather_rows(values, axis):
    for stride in strides_of(axis):
        values = jnp.concatenate([values, swap_with(values, axis, stride)], axis=0)
    return values


def scatter_sum(values, axis):
    for stride in reversed(strides_of(axis)):
        half = values.shape[0] // 2
        other = swap_with(values[half:], axis, stride)
        values = (values[:half].astype(jnp.float32) + other.astype(jnp.float32)).astype(
            values.dtype
        )
    return values


def attend_kernel(heads, scale, q_block, k_block, qn, qp, lat, wk, wv, out, keys, vals, sc, acc):
    rank = wk.shape[0]
    total = lat.shape[0]
    chunks = total // k_block
    half = lax.broadcasted_iota(jnp.int32, (q_block, 2 * NOPE), 1) // NOPE
    part = lax.broadcasted_iota(jnp.int32, (q_block, heads * ROPE), 1) // ROPE

    def project(c, _):
        at = pl.ds(pl.multiple_of(c * k_block, k_block), k_block)
        rows = lat[at, :rank]
        keys[at, :] = jnp.dot(rows, wk[...], preferred_element_type=jnp.float32).astype(keys.dtype)
        vals[at, :] = jnp.dot(rows, wv[...], preferred_element_type=jnp.float32).astype(vals.dtype)
        return 0

    lax.fori_loop(0, chunks, project, 0)

    def one_block(b, _):
        rows = pl.ds(pl.multiple_of(b * q_block, q_block), q_block)
        for pair in range(heads // 2):
            cols = slice(pair * 2 * NOPE, (pair + 1) * 2 * NOPE)
            done = []
            for side in range(2):
                plain = qn[rows, cols]
                plain = jnp.where(half == side, plain, jnp.zeros_like(plain))
                turned = qp[rows, :]
                turned = jnp.where(part == 2 * pair + side, turned, jnp.zeros_like(turned))
                query = jnp.concatenate([plain, turned], axis=1)

                def score(c, peak):
                    at = pl.ds(pl.multiple_of(c * k_block, k_block), k_block)
                    block = jnp.concatenate([keys[at, cols], lat[at, rank:]], axis=1)
                    s = lax.dot_general(
                        query, block, (((1,), (1,)), ((), ())), preferred_element_type=jnp.float32
                    )
                    sc[c] = s
                    for j in range(k_block // 128):
                        peak = jnp.maximum(peak, s[:, j * 128 : (j + 1) * 128])
                    return peak

                peak = lax.fori_loop(
                    0, chunks, score, jnp.full((q_block, 128), -jnp.inf, jnp.float32)
                )
                peak = jnp.max(peak, axis=1, keepdims=True) * (scale * LOG2E)
                acc[...] = jnp.zeros_like(acc)

                def blend(c, _):
                    at = pl.ds(pl.multiple_of(c * k_block, k_block), k_block)
                    w = jnp.exp2(sc[c] * (scale * LOG2E) - peak).astype(jnp.bfloat16)
                    v = vals[at, cols]
                    v = jnp.concatenate([v, jnp.ones_like(v)], axis=1)
                    acc[...] += jnp.dot(w, v, preferred_element_type=jnp.float32)
                    return 0

                lax.fori_loop(0, chunks, blend, 0)
                done.append(acc[:, : 2 * VDIM] / acc[:, 2 * VDIM :])
            out[rows, cols] = jnp.where(half == 0, done[0], done[1]).astype(out.dtype)
        return 0

    lax.fori_loop(0, qn.shape[0] // q_block, one_block, 0)


def attend(query_nope, query_pe, latents, key_plain, value_up):
    rows, width = query_nope.shape
    total = latents.shape[0]
    heads = width // NOPE
    k_block = math.gcd(total, 1024)
    q_block = math.gcd(rows, max(128, min(512, (1 << 21) // total)))
    vmem = pl.BlockSpec(memory_space=pltpu.VMEM)
    pairs = rows * heads * total

    def body(*refs):
        attend_kernel(heads, (NOPE + ROPE) ** (-0.5), q_block, k_block, *refs)

    return pl.pallas_call(
        body,
        out_shape=jax.ShapeDtypeStruct((rows, heads * VDIM), jnp.bfloat16),
        in_specs=[vmem] * 5,
        out_specs=vmem,
        scratch_shapes=[
            pltpu.VMEM((total, width), jnp.bfloat16),
            pltpu.VMEM((total, width), jnp.bfloat16),
            pltpu.VMEM((total // k_block, q_block, k_block), jnp.float32),
            pltpu.VMEM((q_block, 4 * VDIM), jnp.float32),
        ],
        cost_estimate=pl.CostEstimate(
            flops=pairs * 1024, transcendentals=pairs, bytes_accessed=total * 1280
        ),
        name="attend",
    )(query_nope, query_pe, latents, key_plain, value_up)


def on_device(
    mixer_input,
    expert_input,
    mixer_gain,
    query_down,
    latent_down,
    rotary_down,
    query_gain,
    latent_gain,
    query_plain,
    query_rotary,
    key_plain,
    value_up,
    output_proj,
    mixed_gain,
    expert_norm,
    route_ids,
    route_weight,
    gate_proj,
    up_proj,
    down_proj,
    expert_gain,
):
    tok_rows = mixer_input.shape[0]
    groups = lax.axis_size("tp")
    me_tp = lax.axis_index("tp")
    me_ep = lax.axis_index("ep")
    group_base = me_ep * groups * tok_rows
    heads_here = query_plain.shape[1] // NOPE

    expert_hidden = norm_rows(expert_input, expert_norm).astype(jnp.bfloat16)
    experts = lax.axis_size("ep")
    topk = route_ids.shape[1]
    capacity = 5 * tok_rows * topk // (4 * experts)
    slots = experts * capacity
    flat_ids = route_ids.reshape(-1)
    onehot = (flat_ids[:, None] == jnp.arange(experts, dtype=jnp.int32)[None, :]).astype(jnp.int32)
    order = jnp.sum((jnp.cumsum(onehot, axis=0) - onehot) * onehot, axis=1)
    target = (((flat_ids - me_ep) % experts) * capacity + order).reshape(tok_rows, topk)
    slot_ids = jnp.arange(slots, dtype=jnp.int32)
    dispatch = jnp.any(target[None, :, :] == slot_ids[:, None, None], axis=2).astype(jnp.bfloat16)
    width = expert_hidden.shape[1]
    outgoing = (
        jnp.dot(dispatch, expert_hidden, preferred_element_type=jnp.float32)
        .astype(jnp.bfloat16)
        .reshape(experts, capacity, width)
    )
    halves = [range(0, experts // 2), range(experts // 2, experts)]

    def arrive(members):
        blocks = [outgoing[s] if s == 0 else shift_by(outgoing[s], "ep", s) for s in members]
        return gather_rows(jnp.concatenate(blocks, axis=0), "tp")

    arrived = [arrive(members) for members in halves]

    hidden = norm_rows(mixer_input, mixer_gain).astype(jnp.bfloat16)
    own = jnp.array(block_owners("tp"), jnp.int32) ^ me_tp
    positions = (
        group_base + own[:, None] * tok_rows + jnp.arange(tok_rows, dtype=jnp.int32)[None, :]
    ).reshape(-1)
    cosine, sine = turn_tables(positions, ROPE)
    cosine = jnp.concatenate([cosine] * (2 * heads_here), axis=1)
    sine = jnp.concatenate([sine] * (2 * heads_here), axis=1)

    def swapped(weights):
        rows = weights.shape[0]
        parts = weights.reshape(rows, -1, 2, ROPE // 2)
        return jnp.stack([-parts[:, :, 1], parts[:, :, 0]], axis=2).reshape(weights.shape)

    key_lat = norm_rows(
        jnp.dot(hidden, latent_down, preferred_element_type=jnp.float32), latent_gain
    ).astype(jnp.bfloat16)
    turn_w = jnp.concatenate([rotary_down] * heads_here, axis=1)
    turn_w_swapped = jnp.concatenate([swapped(rotary_down)] * heads_here, axis=1)
    key_turn = (
        jnp.dot(hidden, turn_w, preferred_element_type=jnp.float32) * cosine[:tok_rows]
        + jnp.dot(hidden, turn_w_swapped, preferred_element_type=jnp.float32) * sine[:tok_rows]
    ).astype(jnp.bfloat16)
    latents = lax.all_gather(
        jnp.concatenate([key_lat, key_turn], axis=1), ("ep", "tp"), axis=0, tiled=True
    )
    query_lat = norm_rows(
        jnp.dot(hidden, query_down, preferred_element_type=jnp.float32), query_gain
    ).astype(jnp.bfloat16)
    query_rows = gather_rows(query_lat, "tp")
    query_nope = jnp.dot(query_rows, query_plain, preferred_element_type=jnp.float32).astype(
        jnp.bfloat16
    )
    query_pe = (
        jnp.dot(query_rows, query_rotary, preferred_element_type=jnp.float32) * cosine
        + jnp.dot(query_rows, swapped(query_rotary), preferred_element_type=jnp.float32) * sine
    ).astype(jnp.bfloat16)

    gate_w = gate_proj[0]
    up_w = up_proj[0]
    down_w = down_proj[0]

    def expert_rows(rows):
        gate = jnp.minimum(jnp.dot(rows, gate_w, preferred_element_type=jnp.float32), CLAMP)
        up = jnp.clip(jnp.dot(rows, up_w, preferred_element_type=jnp.float32), -CLAMP, CLAMP)
        acts = ((up + 1.0) * gate * jax.nn.sigmoid(ALPHA * gate)).astype(jnp.bfloat16)
        return jnp.dot(acts, down_w, preferred_element_type=jnp.float32).astype(jnp.bfloat16)

    back = []
    for members, rows in zip(halves, arrived):
        sums = scatter_sum(expert_rows(rows), "tp").reshape(len(members), capacity, width)
        back += [
            sums[i] if s == 0 else shift_by(sums[i], "ep", -s) for i, s in enumerate(members)
        ]

    attended = attend(query_nope, query_pe, latents, key_plain, value_up)
    partial = jnp.dot(attended, output_proj, preferred_element_type=jnp.float32).astype(
        jnp.bfloat16
    )
    mixed = scatter_sum(partial, "tp").astype(jnp.float32)
    mixer_out = norm_rows(mixed, mixed_gain).astype(jnp.bfloat16)

    share = jnp.sum(
        jnp.where(target[:, :, None] == slot_ids[None, None, :], route_weight[:, :, None], 0.0),
        axis=1,
    )
    high = share.astype(jnp.bfloat16)
    low = (share - high.astype(jnp.float32)).astype(jnp.bfloat16)
    back_rows = jnp.concatenate(back, axis=0)
    combined = jnp.dot(high, back_rows, preferred_element_type=jnp.float32) + jnp.dot(
        low, back_rows, preferred_element_type=jnp.float32
    )
    expert_out = norm_rows(combined, expert_gain).astype(jnp.bfloat16)
    return (mixer_out, expert_out)


def solution(mesh):
    in_specs = (
        P(("ep", "tp"), None),
        P(("ep", "tp"), None),
        P(),
        P(),
        P(),
        P(),
        P(),
        P(),
        P(None, "tp"),
        P(None, "tp"),
        P(None, "tp"),
        P(None, "tp"),
        P("tp", None),
        P(),
        P(),
        P(("ep", "tp"), None),
        P(("ep", "tp"), None),
        P("ep", None, "tp"),
        P("ep", None, "tp"),
        P("ep", "tp", None),
        P(),
    )
    out_specs = (P(("ep", "tp"), None), P(("ep", "tp"), None))
    return jax.shard_map(
        on_device, mesh=mesh, in_specs=in_specs, out_specs=out_specs, check_vma=False
    )
```

```python
import math

import jax
import jax.numpy as jnp
from jax import lax
from jax.experimental import pallas as pl
from jax.experimental.pallas import tpu as pltpu
from jax.sharding import PartitionSpec as P

NOPE = 64
ROPE = 32
VDIM = 64


EPS = 1e-06
CLAMP = 7.0
ALPHA = 1.702
THETA = 10000.0
LOG2E = math.log2(math.e)


def norm_rows(values, gain):
    values = values.astype(jnp.float32)
    scale = lax.rsqrt(jnp.mean(values * values, axis=-1, keepdims=True) + EPS)
    return values * scale * gain


def turn_tables(positions, width):
    half = width // 2
    freqs = THETA ** (-2.0 * jnp.arange(half, dtype=jnp.float32) / width)
    angles = positions.astype(jnp.float32)[:, None] * freqs[None, :]
    return (jnp.cos(angles), jnp.sin(angles))


def swap_with(values, axis, stride):
    count = lax.axis_size(axis)
    return lax.ppermute(values, axis, [(i, i ^ stride) for i in range(count)])


def shift_by(values, axis, step):
    count = lax.axis_size(axis)
    return lax.ppermute(values, axis, [(i, (i + step) % count) for i in range(count)])


def strides_of(axis):
    count = lax.axis_size(axis)
    return [1 << b for b in reversed(range(count.bit_length() - 1))]


def block_owners(axis):
    owners = [0]
    for stride in strides_of(axis):
        owners = owners + [o ^ stride for o in owners]
    return owners


def gather_rows(values, axis):
    for stride in strides_of(axis):
        values = jnp.concatenate([values, swap_with(values, axis, stride)], axis=0)
    return values


def add_rounded(one, other):
    return (one.astype(jnp.float32) + other.astype(jnp.float32)).astype(one.dtype)


def scatter_sum(values, axis, strides):
    for stride in strides:
        half = values.shape[0] // 2
        other = swap_with(values[half:], axis, stride)
        values = add_rounded(values[:half], other)
    return values


def attend_kernel(heads, scale, q_block, k_block, qn, qp, lat, wk, wv, out, keys, vals, sc, acc):
    rank = wk.shape[0]
    total = lat.shape[0]
    chunks = total // k_block
    half = lax.broadcasted_iota(jnp.int32, (q_block, 2 * NOPE), 1) // NOPE
    part = lax.broadcasted_iota(jnp.int32, (q_block, heads * ROPE), 1) // ROPE

    def project(c, _):
        at = pl.ds(pl.multiple_of(c * k_block, k_block), k_block)
        rows = lat[at, :rank]
        keys[at, :] = jnp.dot(rows, wk[...], preferred_element_type=jnp.float32).astype(keys.dtype)
        vals[at, :] = jnp.dot(rows, wv[...], preferred_element_type=jnp.float32).astype(vals.dtype)
        return 0

    lax.fori_loop(0, chunks, project, 0)

    def one_block(b, _):
        rows = pl.ds(pl.multiple_of(b * q_block, q_block), q_block)
        for pair in range(heads // 2):
            cols = slice(pair * 2 * NOPE, (pair + 1) * 2 * NOPE)
            done = []
            for side in range(2):
                plain = qn[rows, cols]
                plain = jnp.where(half == side, plain, jnp.zeros_like(plain))
                turned = qp[rows, :]
                turned = jnp.where(part == 2 * pair + side, turned, jnp.zeros_like(turned))
                query = jnp.concatenate([plain, turned], axis=1)

                def score(c, peak):
                    at = pl.ds(pl.multiple_of(c * k_block, k_block), k_block)
                    block = jnp.concatenate([keys[at, cols], lat[at, rank:]], axis=1)
                    s = lax.dot_general(
                        query, block, (((1,), (1,)), ((), ())), preferred_element_type=jnp.float32
                    )
                    sc[c] = s
                    for j in range(k_block // 128):
                        peak = jnp.maximum(peak, s[:, j * 128 : (j + 1) * 128])
                    return peak

                peak = lax.fori_loop(
                    0, chunks, score, jnp.full((q_block, 128), -jnp.inf, jnp.float32)
                )
                peak = jnp.max(peak, axis=1, keepdims=True) * (scale * LOG2E)
                acc[...] = jnp.zeros_like(acc)

                def blend(c, _):
                    at = pl.ds(pl.multiple_of(c * k_block, k_block), k_block)
                    w = jnp.exp2(sc[c] * (scale * LOG2E) - peak).astype(jnp.bfloat16)
                    v = vals[at, cols]
                    v = jnp.concatenate([v, jnp.ones_like(v)], axis=1)
                    acc[...] += jnp.dot(w, v, preferred_element_type=jnp.float32)
                    return 0

                lax.fori_loop(0, chunks, blend, 0)
                done.append(acc[:, : 2 * VDIM] / acc[:, 2 * VDIM :])
            out[rows, cols] = jnp.where(half == 0, done[0], done[1]).astype(out.dtype)
        return 0

    lax.fori_loop(0, qn.shape[0] // q_block, one_block, 0)


def attend(query_nope, query_pe, latents, key_plain, value_up):
    rows, width = query_nope.shape
    total = latents.shape[0]
    heads = width // NOPE
    k_block = math.gcd(total, 1024)
    q_block = math.gcd(rows, max(128, min(512, (1 << 21) // total)))
    vmem = pl.BlockSpec(memory_space=pltpu.VMEM)
    pairs = rows * heads * total

    def body(*refs):
        attend_kernel(heads, (NOPE + ROPE) ** (-0.5), q_block, k_block, *refs)

    return pl.pallas_call(
        body,
        out_shape=jax.ShapeDtypeStruct((rows, heads * VDIM), jnp.bfloat16),
        in_specs=[vmem] * 5,
        out_specs=vmem,
        scratch_shapes=[
            pltpu.VMEM((total, width), jnp.bfloat16),
            pltpu.VMEM((total, width), jnp.bfloat16),
            pltpu.VMEM((total // k_block, q_block, k_block), jnp.float32),
            pltpu.VMEM((q_block, 4 * VDIM), jnp.float32),
        ],
        cost_estimate=pl.CostEstimate(
            flops=pairs * 1024, transcendentals=pairs, bytes_accessed=total * 1280
        ),
        name="attend",
    )(query_nope, query_pe, latents, key_plain, value_up)


def on_device(
    mixer_input,
    expert_input,
    mixer_gain,
    query_down,
    latent_down,
    rotary_down,
    query_gain,
    latent_gain,
    query_plain,
    query_rotary,
    key_plain,
    value_up,
    output_proj,
    mixed_gain,
    expert_norm,
    route_ids,
    route_weight,
    gate_proj,
    up_proj,
    down_proj,
    expert_gain,
):
    tok_rows = mixer_input.shape[0]
    groups = lax.axis_size("tp")
    me_tp = lax.axis_index("tp")
    me_ep = lax.axis_index("ep")
    group_base = me_ep * groups * tok_rows
    heads_here = query_plain.shape[1] // NOPE

    expert_hidden = norm_rows(expert_input, expert_norm).astype(jnp.bfloat16)
    experts = lax.axis_size("ep")
    topk = route_ids.shape[1]
    capacity = 5 * tok_rows * topk // (4 * experts)
    slots = experts * capacity
    flat_ids = route_ids.reshape(-1)
    onehot = (flat_ids[:, None] == jnp.arange(experts, dtype=jnp.int32)[None, :]).astype(jnp.int32)
    order = jnp.sum((jnp.cumsum(onehot, axis=0) - onehot) * onehot, axis=1)
    target = (((flat_ids - me_ep) % experts) * capacity + order).reshape(tok_rows, topk)
    slot_ids = jnp.arange(slots, dtype=jnp.int32)
    dispatch = jnp.any(target[None, :, :] == slot_ids[:, None, None], axis=2).astype(jnp.bfloat16)
    width = expert_hidden.shape[1]
    outgoing = (
        jnp.dot(dispatch, expert_hidden, preferred_element_type=jnp.float32)
        .astype(jnp.bfloat16)
        .reshape(experts, capacity, width)
    )
    halves = [range(0, experts // 2), range(experts // 2, experts)]
    outgoing, mixer_input = lax.optimization_barrier((outgoing, mixer_input))

    def arrive(members):
        blocks = [outgoing[s] if s == 0 else shift_by(outgoing[s], "ep", s) for s in members]
        rows = jnp.concatenate(blocks, axis=0)
        for stride in far:
            rows = jnp.concatenate([rows, swap_with(rows, "tp", stride)], axis=0)
        return rows, swap_with(rows, "tp", near)

    *far, near = strides_of("tp")
    arrived = [arrive(members) for members in halves]

    hidden = norm_rows(mixer_input, mixer_gain).astype(jnp.bfloat16)
    own = jnp.array(block_owners("tp"), jnp.int32) ^ me_tp
    positions = (
        group_base + own[:, None] * tok_rows + jnp.arange(tok_rows, dtype=jnp.int32)[None, :]
    ).reshape(-1)
    cosine, sine = turn_tables(positions, ROPE)
    cosine = jnp.concatenate([cosine] * (2 * heads_here), axis=1)
    sine = jnp.concatenate([sine] * (2 * heads_here), axis=1)

    def swapped(weights):
        rows = weights.shape[0]
        parts = weights.reshape(rows, -1, 2, ROPE // 2)
        return jnp.stack([-parts[:, :, 1], parts[:, :, 0]], axis=2).reshape(weights.shape)

    key_lat = norm_rows(
        jnp.dot(hidden, latent_down, preferred_element_type=jnp.float32), latent_gain
    ).astype(jnp.bfloat16)
    turn_w = jnp.concatenate([rotary_down] * heads_here, axis=1)
    turn_w_swapped = jnp.concatenate([swapped(rotary_down)] * heads_here, axis=1)
    key_turn = (
        jnp.dot(hidden, turn_w, preferred_element_type=jnp.float32) * cosine[:tok_rows]
        + jnp.dot(hidden, turn_w_swapped, preferred_element_type=jnp.float32) * sine[:tok_rows]
    ).astype(jnp.bfloat16)
    latents = lax.all_gather(
        jnp.concatenate([key_lat, key_turn], axis=1), ("ep", "tp"), axis=0, tiled=True
    )
    query_lat = norm_rows(
        jnp.dot(hidden, query_down, preferred_element_type=jnp.float32), query_gain
    ).astype(jnp.bfloat16)
    query_rows = gather_rows(query_lat, "tp")
    query_nope = jnp.dot(query_rows, query_plain, preferred_element_type=jnp.float32).astype(
        jnp.bfloat16
    )
    query_pe = (
        jnp.dot(query_rows, query_rotary, preferred_element_type=jnp.float32) * cosine
        + jnp.dot(query_rows, swapped(query_rotary), preferred_element_type=jnp.float32) * sine
    ).astype(jnp.bfloat16)

    gate_w = gate_proj[0]
    up_w = up_proj[0]
    down_w = down_proj[0]

    def expert_rows(rows):
        gate = jnp.minimum(jnp.dot(rows, gate_w, preferred_element_type=jnp.float32), CLAMP)
        up = jnp.clip(jnp.dot(rows, up_w, preferred_element_type=jnp.float32), -CLAMP, CLAMP)
        acts = ((up + 1.0) * gate * jax.nn.sigmoid(ALPHA * gate)).astype(jnp.bfloat16)
        return jnp.dot(acts, down_w, preferred_element_type=jnp.float32).astype(jnp.bfloat16)

    def near_sum(rows):
        here, there = rows
        other = swap_with(expert_rows(there), "tp", near)
        return add_rounded(expert_rows(here), other)

    def far_sum(values, beside=None):
        for stride in reversed(far):
            half = values.shape[0] // 2
            other = swap_with(values[half:], "tp", stride)
            if beside is not None:
                other, beside = lax.optimization_barrier((other, beside))
            values = add_rounded(values[:half], other)
        return values if beside is None else (values, beside)

    def send_back(members, sums):
        sums = sums.reshape(len(members), capacity, width)
        return [sums[i] if s == 0 else shift_by(sums[i], "ep", -s) for i, s in enumerate(members)]

    first, second = arrived
    first_sum = near_sum(first)
    second, first_sum = lax.optimization_barrier((second, first_sum))
    first_sum = far_sum(first_sum)
    second_sum = near_sum(second)
    query_nope, first_sum = lax.optimization_barrier((query_nope, first_sum))
    back = send_back(halves[0], first_sum)
    attended = attend(query_nope, query_pe, latents, key_plain, value_up)
    second_sum, attended = far_sum(second_sum, attended)
    attended, *back = lax.optimization_barrier((attended, *back))
    back += send_back(halves[1], second_sum)
    partial = jnp.dot(attended, output_proj, preferred_element_type=jnp.float32).astype(
        jnp.bfloat16
    )
    rows_sum = scatter_sum(partial, "tp", [near])
    half = rows_sum.shape[0] // 2
    if len(far) == 1:
        other = swap_with(rows_sum[half:], "tp", far[0])
        kept, *back = lax.optimization_barrier((rows_sum[:half], *back))
        mixed = add_rounded(kept, other).astype(jnp.float32)
    else:
        mixed = scatter_sum(rows_sum, "tp", far[::-1]).astype(jnp.float32)
    mixer_out = norm_rows(mixed, mixed_gain).astype(jnp.bfloat16)

    share = jnp.sum(
        jnp.where(target[:, :, None] == slot_ids[None, None, :], route_weight[:, :, None], 0.0),
        axis=1,
    )
    high = share.astype(jnp.bfloat16)
    low = (share - high.astype(jnp.float32)).astype(jnp.bfloat16)
    back_rows = jnp.concatenate(back, axis=0)
    combined = jnp.dot(high, back_rows, preferred_element_type=jnp.float32) + jnp.dot(
        low, back_rows, preferred_element_type=jnp.float32
    )
    expert_out = norm_rows(combined, expert_gain).astype(jnp.bfloat16)
    return (mixer_out, expert_out)


def solution(mesh):
    in_specs = (
        P(("ep", "tp"), None),
        P(("ep", "tp"), None),
        P(),
        P(),
        P(),
        P(),
        P(),
        P(),
        P(None, "tp"),
        P(None, "tp"),
        P(None, "tp"),
        P(None, "tp"),
        P("tp", None),
        P(),
        P(),
        P(("ep", "tp"), None),
        P(("ep", "tp"), None),
        P("ep", None, "tp"),
        P("ep", None, "tp"),
        P("ep", "tp", None),
        P(),
    )
    out_specs = (P(("ep", "tp"), None), P(("ep", "tp"), None))
    return jax.shard_map(
        on_device, mesh=mesh, in_specs=in_specs, out_specs=out_specs, check_vma=False
    )
```
